32 devices in a mesh: ra: 2 (over core), cb: 4 (over z), dp: 4 (over y, x).
Axes of the slice: x: 2, y: 2, z: 4, core: 2. Of those that a mesh axis runs over, the one named last changes fastest.
Arguments:
- residual_in: bfloat16 [1024, 4096], P('dp', 'cb'), may hold values from -220 to 220, as said below
- gain_in: float32 [4096], P('cb'), may hold values from 0.1 to 1.9
- shift_in: float32 [4096], P('cb'), may hold values from -3 to 3
- up_weight: bfloat16 [4096, 16384], P('cb', 'ra'), may hold values from -0.09375 to 0.09375
- down_weight: bfloat16 [16384, 4096], P('ra', 'cb'), may hold values from -0.046875 to 0.046875
- gain_out: float32 [4096], P('cb'), may hold values from 0.1 to 1.9
- shift_out: float32 [4096], P('cb'), may hold values from -3 to 3
Outputs:
- layer_out: bfloat16 [1024, 4096], P('dp', 'cb')
The draws below stay inside these ranges and needn't reach their ends.
Inputs may be any that keep to these rules, and one draw needn't show every extreme that they name: `residual_in`: real-valued activations.
All inputs are finite; a program needn't handle non-finite values.
Results may differ from the reference program's by a relative error of at most 0.0065.
Values may be sent and summed in bfloat16 or wider, within the bound.
No kernel may reach another device: no remote copies, remote signals or barrier semaphores. Data moves between devices by JAX's collectives and lax.ppermute only.
A program may use at most 128 MiB of HBM per device.

```python
import jax
import jax.numpy as jnp
from jax import lax

D = 4096
FF = 16384
TOKENS = 1024


def draw_residual_in(key, part):
    first, second, third = jax.random.split(key, 3)
    column = jnp.arange(D, dtype=jnp.float32) / D
    colscale = 0.5 * jnp.exp(jnp.log(6.0) * column) * jnp.exp(jax.random.uniform(second, (D,), jnp.float32, -0.35, 0.35))
    rowscale = jnp.exp(jax.random.uniform(third, (TOKENS, 1), jnp.float32, 0.0, jnp.log(10.0)))
    noise = jnp.clip(jax.random.normal(first, (TOKENS, D), jnp.float32), -5.0, 5.0)
    values = rowscale * noise * colscale
    return values.astype(jnp.bfloat16)


def steps_of(stream_key, dims, shards, low, high):
    level = 1.0
    for axis_at, parts in shards:
        heights = jax.random.uniform(jax.random.fold_in(jax.random.fold_in(stream_key, 6), axis_at), (parts,), jnp.float32, low / len(shards), high / len(shards))
        level = level * jnp.repeat(jnp.exp(heights), dims[axis_at] // parts).reshape((-1,) + (1,) * (len(dims) - 1 - axis_at))
    return level


def bell_draw(rng, extent, scale, limit, shards=(), kind=jnp.bfloat16):
    level = steps_of(rng, extent, shards, -0.22, 0.18) if shards else 1.0
    values = jax.random.normal(rng, extent, jnp.float32) * scale * level
    return jnp.minimum(jnp.maximum(values, -limit), limit).astype(kind)


def setup_inputs(seed: int = 0) -> dict:
    arg_keys = jax.random.split(jax.random.key(seed), 8)
    residual_in = draw_residual_in(jax.random.fold_in(arg_keys[7], 71), 0)
    gain_in = jnp.clip(1.0 + 0.18 * jax.random.normal(arg_keys[1], (D,), jnp.float32), 0.1, 1.9)
    shift_in = bell_draw(arg_keys[2], (D,), 0.5, 3.0, ((0, 4),), jnp.float32)
    up_weight = bell_draw(arg_keys[3], (D, FF), D ** -0.5, 0.09375, ((0, 4), (1, 2)))
    down_weight = bell_draw(arg_keys[4], (FF, D), FF ** -0.5, 0.046875, ((0, 2), (1, 4)))
    gain_out = jnp.clip(1.0 + 0.18 * jax.random.normal(arg_keys[5], (D,), jnp.float32), 0.1, 1.9)
    shift_out = bell_draw(arg_keys[6], (D,), 0.5, 3.0, ((0, 4),), jnp.float32)
    return {"residual_in": residual_in, "gain_in": gain_in, "shift_in": shift_in, "up_weight": up_weight, "down_weight": down_weight, "gain_out": gain_out, "shift_out": shift_out}


def layer_norm(values, gain, shift):
    mean = lax.optimization_barrier(jnp.mean(values, axis=-1, keepdims=True))
    centred = values - mean
    spread = lax.optimization_barrier(jnp.mean(centred * centred, axis=-1, keepdims=True))
    return centred * jax.lax.rsqrt(spread + 1e-05) * gain + shift

def reference(residual_in, gain_in, shift_in, up_weight, down_weight, gain_out, shift_out):
    normed = layer_norm(residual_in.astype(jnp.float32), gain_in, shift_in).astype(jnp.bfloat16)
    pre = jnp.dot(normed, up_weight, preferred_element_type=jnp.float32)
    hidden = jnp.square(jax.nn.relu(pre)).astype(jnp.bfloat16)
    branch = jnp.dot(hidden, down_weight, preferred_element_type=jnp.float32)
    total = 2.0 ** 0.25 * normed.astype(jnp.float32) + branch
    return layer_norm(total, gain_out, shift_out).astype(jnp.bfloat16)
```

```python
import jax
import jax.numpy as jnp
from jax import lax
from jax.sharding import PartitionSpec as P

PIECES = 16
LAG = 3
EPS = 1e-05


def gathered(values, axis):
    devices = lax.axis_size(axis)
    if devices > 4:
        return lax.all_gather(values, axis)
    shifts = [[(i, (i + by) % devices) for i in range(devices)] for by in range(1, devices)]
    return jnp.stack([values] + [lax.ppermute(values, axis, pairs) for pairs in shifts])


def row_statistics(values, axis):
    devices = lax.axis_size(axis)
    width = values.shape[1]
    mean = jnp.sum(values, axis=1) / width
    centred = values - mean[:, None]
    squares = jnp.sum(centred * centred, axis=1)
    both = gathered(jnp.stack([mean, squares]), axis)
    means = both[:, 0]
    whole_mean = jnp.mean(means, axis=0)
    offsets = means - whole_mean
    whole_squares = jnp.sum(both[:, 1], axis=0) + width * jnp.sum(offsets * offsets, axis=0)
    return whole_mean, whole_squares / (width * devices)


def layer_norm(values, gain, shift):
    mean, spread = row_statistics(values, "cb")
    return (values - mean[:, None]) * lax.rsqrt(spread + EPS)[:, None] * gain + shift


def activate(pre):
    return jnp.square(jax.nn.relu(pre)).astype(jnp.bfloat16)


def feed_forward_line(normed, up_weight, down_weight):
    place = lax.axis_index("cb")
    at_end = jnp.logical_or(place == 0, place == 3)
    inwards, outwards = [(0, 1), (3, 2)], [(1, 0), (2, 3)]
    piece = up_weight.shape[1] // PIECES
    cuts = [slice(at * piece, (at + 1) * piece) for at in range(PIECES)]
    hidden = {}
    branch = 0.0
    for step in range(PIECES + LAG):
        done = step - LAG
        if step < PIECES:
            part = jnp.dot(normed, up_weight[:, cuts[step]], preferred_element_type=jnp.float32)
        if done < 0:
            got = lax.ppermute(part.astype(jnp.bfloat16), "cb", inwards)
        elif step < PIECES:
            sent = jnp.where(at_end, part.astype(jnp.bfloat16), hidden[done])
            got = lax.ppermute(sent, "cb", inwards + outwards)
        else:
            got = lax.ppermute(hidden[done], "cb", outwards)
        if step < PIECES:
            half = part + got.astype(jnp.float32)
            other = lax.ppermute(half.astype(jnp.bfloat16), "cb", [(1, 2), (2, 1)])
            hidden[step] = activate(half + other.astype(jnp.float32))
        if done >= 0:
            whole = jnp.where(at_end, got, hidden[done])
            branch = branch + jnp.dot(
                whole, down_weight[cuts[done]], preferred_element_type=jnp.float32
            )
    return branch


def feed_forward_any(normed, up_weight, down_weight):
    products = jnp.dot(normed, up_weight, preferred_element_type=jnp.float32)
    share = lax.psum_scatter(products, "cb", scatter_dimension=1, tiled=True)
    hidden = lax.all_gather(activate(share), "cb", axis=1, tiled=True)
    return jnp.dot(hidden, down_weight, preferred_element_type=jnp.float32)


def per_device(residual_in, gain_in, shift_in, up_weight, down_weight, gain_out, shift_out):
    normed = layer_norm(residual_in.astype(jnp.float32), gain_in, shift_in).astype(jnp.bfloat16)
    normed = lax.optimization_barrier(normed)
    if lax.axis_size("cb") == 4 and up_weight.shape[1] % PIECES == 0:
        branch_part = feed_forward_line(normed, up_weight, down_weight)
    else:
        branch_part = feed_forward_any(normed, up_weight, down_weight)
    if lax.axis_size("ra") == 2:
        branch = branch_part + lax.ppermute(branch_part, "ra", [(0, 1), (1, 0)])
    else:
        branch = lax.psum(branch_part, "ra")
    total = 2.0**0.25 * normed.astype(jnp.float32) + branch
    return layer_norm(total, gain_out, shift_out).astype(jnp.bfloat16)


def solution(mesh):
    in_specs = (P("dp", "cb"), P("cb"), P("cb"), P("cb", "ra"), P("ra", "cb"), P("cb"), P("cb"))
    out_specs = P("dp", "cb")
    return jax.shard_map(
        per_device, mesh=mesh, in_specs=in_specs, out_specs=out_specs, check_vma=False
    )
```

```python
import functools

import jax
import jax.numpy as jnp
from jax import lax
from jax.experimental import pallas as pl
from jax.experimental.pallas import tpu as pltpu
from jax.sharding import PartitionSpec as P

PIECES = 16
LAG = 4
MIB = 2**20
GROUPS = ((1, 3), (4, 6), (10, 6))
SMALL_GRANT = 8 * MIB
LARGE_GRANT = 50 * MIB
EPS = 1e-05


def gathered(values, axis):
    devices = lax.axis_size(axis)
    if devices > 4:
        return list(lax.all_gather(values, axis))
    shifts = [[(i, (i + by) % devices) for i in range(devices)] for by in range(1, devices)]
    return [values] + [lax.ppermute(values, axis, pairs) for pairs in shifts]


def row_statistics(values, axis):
    devices = lax.axis_size(axis)
    width = values.shape[1]
    mean = jnp.sum(values, axis=1) / width
    centred = values - mean[:, None]
    squares = jnp.sum(centred * centred, axis=1)
    both = jnp.stack(gathered(jnp.stack([mean, squares]), axis))
    means = both[:, 0]
    whole_mean = jnp.mean(means, axis=0)
    offsets = means - whole_mean
    whole_squares = jnp.sum(both[:, 1], axis=0) + width * jnp.sum(offsets * offsets, axis=0)
    return whole_mean, whole_squares / (width * devices)


def layer_norm(values, gain, shift):
    mean, spread = row_statistics(values, "cb")
    return (values - mean[:, None]) * lax.rsqrt(spread + EPS)[:, None] * gain + shift


def activate(pre):
    return jnp.square(jax.nn.relu(pre)).astype(jnp.bfloat16)


def columns_of(first, second):
    lane = lax.broadcasted_iota(jnp.int32, (first.shape[0], 128), 1)
    return jnp.where(lane == 0, first, second).T[:8]


def statistics_kernel(values_ref, out_ref, kept_ref):
    kept_ref[...] = values_ref[...]
    values = values_ref[...].astype(jnp.float32)
    mean = jnp.sum(values, axis=1, keepdims=True) / values.shape[1]
    centred = values - mean
    out_ref[...] = columns_of(mean, jnp.sum(centred * centred, axis=1, keepdims=True))


def statistics(values):
    whole = pl.BlockSpec(memory_space=pltpu.VMEM)
    return pl.pallas_call(
        statistics_kernel,
        in_specs=[whole],
        out_specs=[whole] * 2,
        out_shape=[
            jax.ShapeDtypeStruct((8, values.shape[0]), jnp.float32),
            jax.ShapeDtypeStruct(values.shape, values.dtype),
        ],
        compiler_params=pltpu.CompilerParams(vmem_limit_bytes=SMALL_GRANT),
        name="statistics",
    )(values)


def normalise_kernel(values_ref, *rest):
    stat_refs, rest = rest[:-6], rest[-6:]
    affine_ref, weight_ref, normed_ref, part_ref, held, semaphore = rest
    copy = pltpu.make_async_copy(weight_ref.at[:, : held.shape[1]], held, semaphore)
    copy.start()
    width = values_ref.shape[1]
    stats = [ref[...] for ref in stat_refs]
    mean = sum(one[0:1] for one in stats) / len(stats)
    squares = sum(one[1:2] + width * jnp.square(one[0:1] - mean) for one in stats)
    scale = lax.rsqrt(squares / (width * len(stats)) + EPS)
    row = lax.broadcasted_iota(jnp.int32, (128, mean.shape[1]), 0)
    columns = jnp.where(row == 0, mean, scale).T
    values = values_ref[...].astype(jnp.float32)
    normed = (values - columns[:, 0:1]) * columns[:, 1:2] * affine_ref[0:1] + affine_ref[1:2]
    normed_ref[...] = normed.astype(normed_ref.dtype)
    copy.wait()
    part_ref[...] = jnp.dot(
        normed_ref[...], held[...], preferred_element_type=jnp.float32
    ).astype(part_ref.dtype)


def normalise(values, stats, affine, weight, piece):
    tokens, width = values.shape
    whole = pl.BlockSpec(memory_space=pltpu.VMEM)
    return pl.pallas_call(
        normalise_kernel,
        in_specs=[whole] * (len(stats) + 2) + [pl.BlockSpec(memory_space=pltpu.HBM)],
        out_specs=[whole] * 2,
        out_shape=[
            jax.ShapeDtypeStruct((tokens, width), jnp.bfloat16),
            jax.ShapeDtypeStruct((tokens, piece), jnp.bfloat16),
        ],
        scratch_shapes=[pltpu.VMEM((width, piece), weight.dtype), pltpu.SemaphoreType.DMA],
        compiler_params=pltpu.CompilerParams(vmem_limit_bytes=LARGE_GRANT),
        name="normalise",
    )(values, *stats, affine, weight)


def up_kernel(first, rows_ref, weight_ref, *rest):
    out_refs, (held, semaphores) = rest[:-2], rest[-2:]
    copies = []
    for at in range(len(out_refs)):
        columns = pl.ds((first + at) * held.shape[2], held.shape[2])
        copies.append(
            pltpu.make_async_copy(weight_ref.at[:, columns], held.at[at], semaphores.at[at])
        )
        copies[at].start()
    for at, out_ref in enumerate(out_refs):
        copies[at].wait()
        product = jnp.dot(rows_ref[...], held[at], preferred_element_type=jnp.float32)
        out_ref[...] = product.astype(out_ref.dtype)


def up_pieces(rows, weight, first, count, piece):
    tokens, depth = rows.shape
    whole = pl.BlockSpec(memory_space=pltpu.VMEM)
    held = 2 * depth * piece * count
    moved = 2 * tokens * (depth + piece * count)
    return pl.pallas_call(
        functools.partial(up_kernel, first),
        in_specs=[whole, pl.BlockSpec(memory_space=pltpu.HBM)],
        out_specs=[whole] * count,
        out_shape=[jax.ShapeDtypeStruct((tokens, piece), jnp.bfloat16)] * count,
        scratch_shapes=[
            pltpu.VMEM((count, depth, piece), weight.dtype),
            pltpu.SemaphoreType.DMA((count,)),
        ],
        compiler_params=pltpu.CompilerParams(vmem_limit_bytes=LARGE_GRANT),
        cost_estimate=pl.CostEstimate(
            flops=2 * tokens * depth * piece * count,
            bytes_accessed=held + moved,
            transcendentals=0,
        ),
    )(rows, weight)


def feed_forward_line(residual_in, gain_in, shift_in, up_weight, down_weight):
    place = lax.axis_index("cb")
    at_end = jnp.logical_or(place == 0, place == 3)
    inwards, outwards = [(0, 1), (3, 2)], [(1, 0), (2, 3)]
    piece = up_weight.shape[1] // PIECES
    own, kept = statistics(residual_in)
    stats = gathered(own, "cb")
    affine = jnp.stack([gain_in, shift_in])
    normed, part = normalise(kept, stats, affine, up_weight, piece)
    parts = [part]
    for first, count in GROUPS:
        parts += up_pieces(normed, up_weight, first, count, piece)
    hidden = {}
    branch = None
    for step in range(PIECES + LAG):
        done = step - LAG
        if done < 0:
            sent, pairs = parts[step], inwards
        elif step < PIECES:
            sent = jnp.where(at_end, parts[step], hidden[done])
            pairs = inwards + outwards
        else:
            sent, pairs = hidden[done], outwards
        got = lax.ppermute(sent, "cb", pairs)
        if step < PIECES:
            half = parts[step].astype(jnp.float32) + got.astype(jnp.float32)
            rounded_half = half.astype(jnp.bfloat16)
            other = lax.ppermute(rounded_half, "cb", [(1, 2), (2, 1)])
            hidden[step] = activate(half + other.astype(jnp.float32))
        if done >= 0:
            whole = jnp.where(at_end, got, hidden[done])
            product = jnp.dot(whole, down_weight[done * piece : (done + 1) * piece], preferred_element_type=jnp.float32)
            if done == PIECES - 1:
                return normed, branch, product
            branch = lax.optimization_barrier(product if done == 0 else branch + product)


def feed_forward_any(normed, up_weight, down_weight):
    products = jnp.dot(normed, up_weight, preferred_element_type=jnp.float32)
    share = lax.psum_scatter(products, "cb", scatter_dimension=1, tiled=True)
    hidden = lax.all_gather(activate(share), "cb", axis=1, tiled=True)
    return jnp.dot(hidden, down_weight, preferred_element_type=jnp.float32)


def per_device(residual_in, gain_in, shift_in, up_weight, down_weight, gain_out, shift_out):
    sizes = {axis: lax.axis_size(axis) for axis in ("ra", "cb")}
    if sizes == {"ra": 2, "cb": 4} and up_weight.shape[1] % (128 * PIECES) == 0:
        normed, most, last = feed_forward_line(
            residual_in, gain_in, shift_in, up_weight, down_weight
        )
        swap = functools.partial(lax.ppermute, axis_name="ra", perm=[(0, 1), (1, 0)])
        last = last.astype(jnp.bfloat16)
        total = 2.0**0.25 * normed.astype(jnp.float32) + (most + swap(most))
        total = total + (last.astype(jnp.float32) + swap(last).astype(jnp.float32))
    else:
        normed = layer_norm(residual_in.astype(jnp.float32), gain_in, shift_in)
        normed = normed.astype(jnp.bfloat16)
        branch = lax.psum(feed_forward_any(normed, up_weight, down_weight), "ra")
        total = 2.0**0.25 * normed.astype(jnp.float32) + branch
    return layer_norm(total, gain_out, shift_out).astype(jnp.bfloat16)


def solution(mesh):
    in_specs = (P("dp", "cb"), P("cb"), P("cb"), P("cb", "ra"), P("ra", "cb"), P("cb"), P("cb"))
    out_specs = P("dp", "cb")
    return jax.shard_map(
        per_device, mesh=mesh, in_specs=in_specs, out_specs=out_specs, check_vma=False
    )
```

```python
import functools

import jax
import jax.numpy as jnp
from jax import lax
from jax.experimental import pallas as pl
from jax.experimental.pallas import tpu as pltpu
from jax.sharding import PartitionSpec as P

PIECES = 16
LANES = 128
LAG = 4
MIB = 2**20
GROUPS = ((1, 3), (4, 6), (10, 6))
SMALL_GRANT = 8 * MIB
LARGE_GRANT = 50 * MIB
EPS = 1e-05


def gathered(values, axis):
    devices = lax.axis_size(axis)
    if devices != 4:
        return list(lax.all_gather(values, axis))
    shifts = [[(i, (i + by) % devices) for i in range(devices)] for by in range(1, devices)]
    return [values] + [lax.ppermute(values, axis, pairs) for pairs in shifts]


def row_statistics(values, axis):
    devices = lax.axis_size(axis)
    width = values.shape[1]
    mean = jnp.sum(values, axis=1) / width
    centred = values - mean[:, None]
    squares = jnp.sum(centred * centred, axis=1)
    both = jnp.stack(gathered(jnp.stack([mean, squares]), axis))
    means = both[:, 0]
    whole_mean = jnp.mean(means, axis=0)
    offsets = means - whole_mean
    whole_squares = jnp.sum(both[:, 1], axis=0) + width * jnp.sum(offsets * offsets, axis=0)
    return whole_mean, whole_squares / (width * devices)


def layer_norm(values, gain, shift):
    mean, spread = row_statistics(values, "cb")
    return (values - mean[:, None]) * lax.rsqrt(spread + EPS)[:, None] * gain + shift


def activate(pre):
    return jnp.square(jax.nn.relu(pre)).astype(jnp.bfloat16)


def columns_of(first, second):
    lane = lax.broadcasted_iota(jnp.int32, (first.shape[0], 128), 1)
    return jnp.where(lane == 0, first, second).T[:8]


def statistics_kernel(values_ref, out_ref, kept_ref):
    kept_ref[...] = values_ref[...]
    values = values_ref[...].astype(jnp.float32)
    mean = jnp.sum(values, axis=1, keepdims=True) / values.shape[1]
    centred = values - mean
    out_ref[...] = columns_of(mean, jnp.sum(centred * centred, axis=1, keepdims=True))


def statistics(values):
    whole = pl.BlockSpec(memory_space=pltpu.VMEM)
    return pl.pallas_call(
        statistics_kernel,
        in_specs=[whole],
        out_specs=[whole] * 2,
        out_shape=[
            jax.ShapeDtypeStruct((8, values.shape[0]), jnp.float32),
            jax.ShapeDtypeStruct(values.shape, values.dtype),
        ],
        compiler_params=pltpu.CompilerParams(vmem_limit_bytes=SMALL_GRANT),
        name="statistics",
    )(values)


def normalise_kernel(values_ref, *rest):
    stat_refs, rest = rest[:-6], rest[-6:]
    affine_ref, weight_ref, normed_ref, part_ref, held, semaphore = rest
    copy = pltpu.make_async_copy(weight_ref.at[:, : held.shape[1]], held, semaphore)
    copy.start()
    width = values_ref.shape[1]
    stats = [ref[...] for ref in stat_refs]
    mean = sum(one[0:1] for one in stats) / len(stats)
    squares = sum(one[1:2] + width * jnp.square(one[0:1] - mean) for one in stats)
    scale = lax.rsqrt(squares / (width * len(stats)) + EPS)
    row = lax.broadcasted_iota(jnp.int32, (128, mean.shape[1]), 0)
    columns = jnp.where(row == 0, mean, scale).T
    values = values_ref[...].astype(jnp.float32)
    normed = (values - columns[:, 0:1]) * columns[:, 1:2] * affine_ref[0:1] + affine_ref[1:2]
    normed_ref[...] = normed.astype(normed_ref.dtype)
    copy.wait()
    part_ref[...] = jnp.dot(
        normed_ref[...], held[...], preferred_element_type=jnp.float32
    ).astype(part_ref.dtype)


def normalise(values, stats, affine, weight, piece):
    tokens, width = values.shape
    whole = pl.BlockSpec(memory_space=pltpu.VMEM)
    return pl.pallas_call(
        normalise_kernel,
        in_specs=[whole] * (len(stats) + 2) + [pl.BlockSpec(memory_space=pltpu.HBM)],
        out_specs=[whole] * 2,
        out_shape=[
            jax.ShapeDtypeStruct((tokens, width), jnp.bfloat16),
            jax.ShapeDtypeStruct((tokens, piece), jnp.bfloat16),
        ],
        scratch_shapes=[pltpu.VMEM((width, piece), weight.dtype), pltpu.SemaphoreType.DMA],
        compiler_params=pltpu.CompilerParams(vmem_limit_bytes=LARGE_GRANT),
        name="normalise",
    )(values, *stats, affine, weight)


def up_kernel(cuts, rows_ref, weight_ref, *rest):
    out_refs, (held, semaphores) = rest[:-2], rest[-2:]
    base = cuts[0].start
    places = [pl.ds(cut.start - base, cut.stop - cut.start) for cut in cuts]
    copies = []
    for at, (cut, place) in enumerate(zip(cuts, places)):
        columns = pl.ds(cut.start, cut.stop - cut.start)
        copies.append(
            pltpu.make_async_copy(
                weight_ref.at[:, columns], held.at[:, place], semaphores.at[at]
            )
        )
        copies[at].start()
    for at, out_ref in enumerate(out_refs):
        copies[at].wait()
        product = jnp.dot(rows_ref[...], held[:, places[at]], preferred_element_type=jnp.float32)
        out_ref[...] = product.astype(out_ref.dtype)


def up_pieces(rows, weight, cuts):
    tokens, depth = rows.shape
    columns = cuts[-1].stop - cuts[0].start
    whole = pl.BlockSpec(memory_space=pltpu.VMEM)
    return pl.pallas_call(
        functools.partial(up_kernel, cuts),
        in_specs=[whole, pl.BlockSpec(memory_space=pltpu.HBM)],
        out_specs=[whole] * len(cuts),
        out_shape=[
            jax.ShapeDtypeStruct((tokens, cut.stop - cut.start), jnp.bfloat16) for cut in cuts
        ],
        scratch_shapes=[
            pltpu.VMEM((depth, columns), weight.dtype),
            pltpu.SemaphoreType.DMA((len(cuts),)),
        ],
        compiler_params=pltpu.CompilerParams(vmem_limit_bytes=LARGE_GRANT),
        cost_estimate=pl.CostEstimate(
            flops=2 * tokens * depth * columns,
            bytes_accessed=2 * (tokens * depth + depth * columns + tokens * columns),
            transcendentals=0,
        ),
        name="up",
    )(rows, weight)


def cuts_of(units):
    lanes, uses = units // LANES, [len(range(at, PIECES, LAG)) for at in range(LAG)]
    widths, at = [-(-lanes // PIECES)] * LAG, LAG
    while at > 0 and sum(use * width for use, width in zip(uses, widths)) > lanes:
        at -= 1
        widths[at] -= 1
    if units % LANES or sum(use * width for use, width in zip(uses, widths)) != lanes:
        return None
    ends = [0]
    for at in range(PIECES):
        ends.append(ends[-1] + widths[at % LAG] * LANES)
    return [slice(low, high) for low, high in zip(ends, ends[1:])]


def feed_forward_line(residual_in, gain_in, shift_in, up_weight, down_weight):
    place = lax.axis_index("cb")
    at_end = jnp.logical_or(place == 0, place == 3)
    inwards, outwards = [(0, 1), (3, 2)], [(1, 0), (2, 3)]
    cuts = cuts_of(up_weight.shape[1])
    own, kept = statistics(residual_in)
    stats = gathered(own, "cb")
    affine = jnp.stack([gain_in, shift_in])
    normed, part = normalise(kept, stats, affine, up_weight, cuts[0].stop)
    parts = [part]
    for first, count in GROUPS:
        parts += up_pieces(normed, up_weight, cuts[first : first + count])
    hidden = {}
    branch = None
    for step in range(PIECES + LAG):
        done = step - LAG
        if done < 0:
            sent, pairs = parts[step], inwards
        elif step < PIECES:
            sent = jnp.where(at_end, parts[step], hidden[done])
            pairs = inwards + outwards
        else:
            sent, pairs = hidden[done], outwards
        got = lax.ppermute(sent, "cb", pairs)
        if step < PIECES:
            half = parts[step].astype(jnp.float32) + got.astype(jnp.float32)
            rounded_half = half.astype(jnp.bfloat16)
            other = lax.ppermute(rounded_half, "cb", [(1, 2), (2, 1)])
            hidden[step] = activate(half + other.astype(jnp.float32))
        if done >= 0:
            whole = jnp.where(at_end, got, hidden[done])
            product = jnp.dot(whole, down_weight[cuts[done]], preferred_element_type=jnp.float32)
            if done == PIECES - 1:
                return normed, branch, product
            branch = lax.optimization_barrier(product if done == 0 else branch + product)


def feed_forward_any(normed, up_weight, down_weight):
    products = jnp.dot(normed, up_weight, preferred_element_type=jnp.float32)
    share = lax.psum_scatter(products, "cb", scatter_dimension=1, tiled=True)
    hidden = lax.all_gather(activate(share), "cb", axis=1, tiled=True)
    return jnp.dot(hidden, down_weight, preferred_element_type=jnp.float32)


def per_device(residual_in, gain_in, shift_in, up_weight, down_weight, gain_out, shift_out):
    sizes = {axis: lax.axis_size(axis) for axis in ("ra", "cb")}
    if sizes == {"ra": 2, "cb": 4} and cuts_of(up_weight.shape[1]):
        normed, most, last = feed_forward_line(
            residual_in, gain_in, shift_in, up_weight, down_weight
        )
        swap = functools.partial(lax.ppermute, axis_name="ra", perm=[(0, 1), (1, 0)])
        last = last.astype(jnp.bfloat16)
        total = 2.0**0.25 * normed.astype(jnp.float32) + (most + swap(most))
        total = lax.optimization_barrier(total)
        total = total + (last.astype(jnp.float32) + swap(last).astype(jnp.float32))
    else:
        normed = layer_norm(residual_in.astype(jnp.float32), gain_in, shift_in)
        normed = normed.astype(jnp.bfloat16)
        branch = lax.psum(feed_forward_any(normed, up_weight, down_weight), "ra")
        total = 2.0**0.25 * normed.astype(jnp.float32) + branch
    return layer_norm(total, gain_out, shift_out).astype(jnp.bfloat16)


def solution(mesh):
    in_specs = (P("dp", "cb"), P("cb"), P("cb"), P("cb", "ra"), P("ra", "cb"), P("cb"), P("cb"))
    out_specs = P("dp", "cb")
    return jax.shard_map(
        per_device, mesh=mesh, in_specs=in_specs, out_specs=out_specs, check_vma=False
    )
```
